32 devices in a mesh: grp: 2 (over x), ep: 16 (over z, y, core).
Axes of the slice: x: 2, y: 2, z: 4, core: 2. Of those that a mesh axis runs over, the one named last changes fastest.
Arguments:
- tokens: bfloat16 [1024, 2048], P(('grp', 'ep')), parts along dimension 0, may hold values from -6 to 6
- routes: int32 [1024, 4], P(('grp', 'ep')), parts along dimension 0, may hold values from 0 to 15, all different within a row; in each aligned block of 32 rows (0 to 31, 32 to 63, ...) at most 16 rows name the same one
- route_logits: float32 [1024, 4], P(('grp', 'ep')), parts along dimension 0, may hold values from -4 to 4
- state_real: float32 [1024, 64, 64], P('grp', 'ep'), parts along dimension 0, may hold values from -4 to 4
- state_imag: float32 [1024, 64, 64], P('grp', 'ep'), parts along dimension 0, may hold values from -4 to 4
- gain_in: float32 [2048], replicated, may hold values from 0.1 to 1.9
- proj_in: bfloat16 [2048, 1024], P(None, 'ep'), may hold values from -0.125 to 0.125
- decay_rate: float32 [64, 64], P('ep'), may hold values from 0.05 to 2
- frequency: float32 [64, 64], P('ep'), may hold values from -4 to 4
- log_step: float32 [64], P('ep'), may hold values from -3 to 0
- input_real: float32 [64, 64, 16], P('ep'), may hold values from -1 to 1
- input_imag: float32 [64, 64, 16], P('ep'), may hold values from -1 to 1
- output_real: float32 [64, 16, 64], P('ep'), may hold values from -0.5 to 0.5
- output_imag: float32 [64, 16, 64], P('ep'), may hold values from -0.5 to 0.5
- skip_gain: float32 [64, 16], P('ep'), may hold values from -4 to 4
- proj_out: bfloat16 [1024, 2048], P('ep'), may hold values from -0.1875 to 0.1875
- gain_mid: float32 [2048], replicated, may hold values from 0.1 to 1.9
- expert_gate: bfloat16 [16, 2048, 1024], P('ep'), may hold values from -0.33007812 to 0.33007812
- expert_up: bfloat16 [16, 2048, 1024], P('ep'), may hold values from -0.33007812 to 0.33007812
- expert_down: bfloat16 [16, 1024, 2048], P('ep'), may hold values from -0.056152344 to 0.056152344
- dense_gate: bfloat16 [2048, 2048], P(None, 'ep'), may hold values from -0.125 to 0.125
- dense_up: bfloat16 [2048, 2048], P(None, 'ep'), may hold values from -0.125 to 0.125
- dense_down: bfloat16 [2048, 2048], P('ep'), may hold values from -0.125 to 0.125
- dense_mix: float32 [2048], P('ep'), may hold values from -0.39774758 to 0.39774758
Outputs:
- layer_out: bfloat16 [1024, 2048], P(('grp', 'ep')), parts along dimension 0
- state_real_new: float32 [1024, 64, 64], P('grp', 'ep'), parts along dimension 0
- state_imag_new: float32 [1024, 64, 64], P('grp', 'ep'), parts along dimension 0
The draws below stay inside these ranges and needn't reach their ends.
There are 2 independent parts, one for each index of `grp`. The reference program is written for one: setup_inputs(seed, part) draws one part's arguments, and reference() takes and returns one part's arrays. A program takes and returns all parts, laid end to end along the dimension named above; an argument that names none is the same for every part. Nothing has to cross between parts.
Inputs may be any that keep to these rules, and one draw needn't show every extreme that they name: `routes`: each row names 4 different experts; among the rows of one device no expert is named more than 16 times, and in every draw some device names some expert exactly 16 times.
All inputs are finite; a program needn't handle non-finite values.
Results may differ from the reference program's by a relative error of at most 0.015.
Values may be sent and summed in bfloat16 or wider, within the bound.
A program may use at most 128 MiB of HBM per device.

```python
import math
import jax
import jax.numpy as jnp
import numpy as np
from jax import lax

D = 2048
CHANNELS = 1024
GROUP = 16
GROUPS = 64
STATE = 64
FF = 1024
DENSE = 2048
TOPK = 4
EXPERTS = 16
SEQ_DEV = 32
SEQS = 512
CAP = 16
N_EP = 16


def block_scale(key, shape, split, smallest, top_value):
    def one(axis_at, parts):
        steps = jax.random.uniform(jax.random.fold_in(jax.random.fold_in(key, 6), axis_at), (parts,), jnp.float32, smallest / len(split), top_value / len(split))
        return jnp.repeat(jnp.exp(steps), shape[axis_at] // parts).reshape((-1,) + (1,) * (len(shape) - axis_at - 1))

    gain = one(*split[0])
    for cut in split[1:]:
        gain = gain * one(*cut)
    return gain


def assign_block(key, own, number, rows, count, top, most, slope):
    sequence = jax.random.permutation(key, count)
    heavy_load, ordinary = load_shares(count, rows * top, most, slope, True), load_shares(count, rows * top, most, slope, False)
    places = jnp.arange(count)

    def named(lengths, rotation):
        used = int((lengths > 0).sum())
        fixed = max(1, used // 4)
        moved = fixed + (places - fixed + rotation * (used - fixed)) % max(1, count - fixed)
        return jnp.zeros((count,), jnp.int32).at[sequence[jnp.where(places < fixed, places, moved)]].set(jnp.asarray(lengths, jnp.int32))

    lengths = jnp.where(number % 4 == 0, named(heavy_load, number // 4), named(ordinary, number - number // 4 - 1))
    mixed = jax.random.permutation(jax.random.fold_in(own, 3), count)
    source_of, taker = mixed[0:count // 2 * 2:2], mixed[1:count // 2 * 2:2]
    slack = jnp.minimum(lengths[source_of] - 1, most - lengths[taker]) // 2
    slack = jnp.where((source_of == sequence[0]) | (taker == sequence[0]) | (lengths[taker] == 0), 0, jnp.maximum(slack, 0))
    moved = jax.random.randint(jax.random.fold_in(own, 4), (count // 2,), 0, 1 << 20) % (slack + 1)
    lengths = lengths.at[source_of].add(-moved).at[taker].add(moved)
    labels = jnp.searchsorted(jnp.cumsum(lengths), jnp.arange(rows * top), side="right").astype(jnp.int32)
    table = labels.reshape(top, rows).T
    table = table[jax.random.permutation(jax.random.fold_in(own, 1), rows)]
    rotation = jax.random.randint(jax.random.fold_in(own, 2), (rows, 1), 0, top)
    return jnp.take_along_axis(table, (jnp.arange(top)[None, :] + rotation) % top, axis=1)


def load_shares(amount, total, limit, skew, full):
    loads = [(1 << 20) // math.isqrt(grade ** skew) + 1 for grade in range(1, amount + 1)]
    largest = limit if full else min(limit, max(-(-total // amount), total * loads[0] // sum(loads)))
    least = 1 if total - largest >= amount - 1 else 0
    given, rest = [largest] + [least] * (amount - 1), total - largest - least * (amount - 1)
    while rest > 0:
        candidates = [i for i in range(1, amount) if given[i] < largest] or [i for i in range(1, amount) if given[i] < limit]
        mass, remaining = sum([loads[i] for i in candidates]), rest
        for i in candidates:
            addition = min(limit - given[i], max(1, remaining * loads[i] // mass), rest)
            given[i] = given[i] + addition
            rest = rest - addition
    return np.array(given)


def gaussian(own_key, extent, spread, most, shards=(), kind=jnp.bfloat16):
    loudness = block_scale(own_key, extent, shards, -0.22, 0.18) if shards else 1.0
    entries = jax.random.normal(own_key, extent, jnp.float32) * spread * loudness
    return jnp.minimum(jnp.maximum(entries, -most), most).astype(kind)


def setup_inputs(seed: int = 0, part: int = 0) -> dict:
    splits = jax.random.split(jax.random.key(seed), 25)
    part_keys = jax.random.split(jax.random.fold_in(splits[24], part), 25)
    tokens = gaussian(part_keys[0], (SEQS, D), 1.0, 6.0, ((0, 16),))
    routes_keys = jax.random.split(jax.random.fold_in(part_keys[1], 1), SEQS // SEQ_DEV)
    routes_turns = jax.random.permutation(jax.random.fold_in(part_keys[1], 3), SEQS // SEQ_DEV)
    routes = jax.vmap(lambda own, number: assign_block(jax.random.fold_in(part_keys[1], 2), own, number, SEQ_DEV, EXPERTS, TOPK, CAP, 2))(routes_keys, routes_turns).reshape((SEQS, TOPK))
    route_logits = gaussian(part_keys[2], (SEQS, TOPK), 1.0, 4.0, ((0, 16),), jnp.float32)
    state_real = gaussian(part_keys[3], (SEQS, GROUPS, STATE), 0.5, 4.0, ((1, 16),), jnp.float32)
    state_imag = gaussian(part_keys[4], (SEQS, GROUPS, STATE), 0.5, 4.0, ((1, 16),), jnp.float32)
    gain_in = jnp.clip(1.0 + 0.18 * jax.random.normal(splits[5], (D,), jnp.float32), 0.1, 1.9)
    proj_in = gaussian(splits[6], (D, CHANNELS), D ** -0.5, 0.125, ((1, 16),))
    decay_rate = jnp.clip(jnp.exp(math.log(2.0) - 3.6888794 * jax.random.uniform(splits[7], (GROUPS, STATE), jnp.float32) ** block_scale(splits[7], (GROUPS, STATE), ((0, 16),), -0.2, 0.2)), 0.05, 2.0)
    frequency = jnp.clip(jax.random.uniform(splits[8], (GROUPS, STATE), jnp.float32, -4.0, 4.0) * block_scale(splits[8], (GROUPS, STATE), ((0, 16),), -0.4, 0.0), -4.0, 4.0)
    log_step = jnp.clip(-3.0 + 3.0 * jax.random.uniform(splits[9], (GROUPS,), jnp.float32) ** block_scale(splits[9], (GROUPS,), ((0, 16),), -0.2, 0.2), -3.0, 0.0)
    input_real = gaussian(splits[10], (GROUPS, STATE, GROUP), (2 * GROUP) ** -0.5, 1.0, ((0, 16),), jnp.float32)
    input_imag = gaussian(splits[11], (GROUPS, STATE, GROUP), (2 * GROUP) ** -0.5, 1.0, ((0, 16),), jnp.float32)
    output_real = gaussian(splits[12], (GROUPS, GROUP, STATE), (2 * STATE) ** -0.5, 0.5, ((0, 16),), jnp.float32)
    output_imag = gaussian(splits[13], (GROUPS, GROUP, STATE), (2 * STATE) ** -0.5, 0.5, ((0, 16),), jnp.float32)
    skip_gain = gaussian(splits[14], (GROUPS, GROUP), 1.0, 4.0, ((0, 16),), jnp.float32)
    proj_out = gaussian(splits[15], (CHANNELS, D), CHANNELS ** -0.5, 0.1875, ((0, 16),))
    gain_mid = jnp.clip(1.0 + 0.18 * jax.random.normal(splits[16], (D,), jnp.float32), 0.1, 1.9)
    expert_gate = gaussian(splits[17], (EXPERTS, D, FF), (2.5 / D ** 0.5), 0.33007812, ((0, 16),))
    expert_up = gaussian(splits[18], (EXPERTS, D, FF), (2.5 / D ** 0.5), 0.33007812, ((0, 16),))
    expert_down = gaussian(splits[19], (EXPERTS, FF, D), (0.3 / FF ** 0.5), 0.056152344, ((0, 16),))
    dense_gate = gaussian(splits[20], (D, DENSE), D ** -0.5, 0.125, ((1, 16),))
    dense_up = gaussian(splits[21], (D, DENSE), D ** -0.5, 0.125, ((1, 16),))
    dense_down = gaussian(splits[22], (DENSE, D), DENSE ** -0.5, 0.125, ((0, 16),))
    dense_mix = gaussian(splits[23], (DENSE,), (3.0 / DENSE ** 0.5), 0.39774758, ((0, 16),), jnp.float32)
    return {"tokens": tokens, "routes": routes, "route_logits": route_logits, "state_real": state_real, "state_imag": state_imag, "gain_in": gain_in, "proj_in": proj_in, "decay_rate": decay_rate, "frequency": frequency, "log_step": log_step, "input_real": input_real, "input_imag": input_imag, "output_real": output_real, "output_imag": output_imag, "skip_gain": skip_gain, "proj_out": proj_out, "gain_mid": gain_mid, "expert_gate": expert_gate, "expert_up": expert_up, "expert_down": expert_down, "dense_gate": dense_gate, "dense_up": dense_up, "dense_down": dense_down, "dense_mix": dense_mix}


EPS = 1e-06
LIMIT = 7.0
ALPHA = 1.702
HIGH = lax.Precision.HIGHEST

def rms_scale(values, gain_vec):
    return values * lax.rsqrt(lax.optimization_barrier(jnp.mean(values * values, axis=-1, keepdims=True)) + EPS) * gain_vec

def state_step(unit_rows, state_real, state_imag, decay_rate, frequency, log_step, input_real, input_imag, output_real, output_imag, skip_gain):
    seq_count = unit_rows.shape[0]
    groups, group_size = skip_gain.shape
    inputs = unit_rows.astype(jnp.float32).reshape(seq_count, groups, group_size)
    step_size = jnp.exp(log_step)[:, None]
    decay_part = -decay_rate
    magnitude = jnp.exp(decay_part * step_size)
    carry_real = magnitude * jnp.cos(frequency * step_size)
    carry_imag = magnitude * jnp.sin(frequency * step_size)
    denom = decay_part * decay_part + frequency * frequency
    feed_real = ((carry_real - 1.0) * decay_part + carry_imag * frequency) / denom
    feed_imag = (carry_imag * decay_part - (carry_real - 1.0) * frequency) / denom
    drive_real = jnp.einsum('sgp,gnp->sgn', inputs, input_real, precision=HIGH)
    drive_imag = jnp.einsum('sgp,gnp->sgn', inputs, input_imag, precision=HIGH)
    new_real = carry_real * state_real - carry_imag * state_imag + feed_real * drive_real - feed_imag * drive_imag
    new_imag = carry_real * state_imag + carry_imag * state_real + feed_real * drive_imag + feed_imag * drive_real
    readout = jnp.einsum('gpn,sgn->sgp', output_real, new_real, precision=HIGH) - jnp.einsum('gpn,sgn->sgp', output_imag, new_imag, precision=HIGH) + skip_gain * inputs
    branch = jax.nn.gelu(readout).reshape(seq_count, groups * group_size).astype(jnp.bfloat16)
    return (branch, new_real, new_imag)

def expert_apply(row_block, gate_weight, up_weight, down_weight):
    gated = jnp.minimum(jnp.dot(row_block, gate_weight, preferred_element_type=jnp.float32), LIMIT)
    upper = jnp.clip(jnp.dot(row_block, up_weight, preferred_element_type=jnp.float32), -LIMIT, LIMIT)
    activated = ((upper + 1.0) * gated * jax.nn.sigmoid(ALPHA * gated)).astype(jnp.bfloat16)
    return jnp.dot(activated, down_weight, preferred_element_type=jnp.float32).astype(jnp.bfloat16)

def reference(tokens, routes, route_logits, state_real, state_imag, gain_in, proj_in, decay_rate, frequency, log_step, input_real, input_imag, output_real, output_imag, skip_gain, proj_out, gain_mid, expert_gate, expert_up, expert_down, dense_gate, dense_up, dense_down, dense_mix):
    inputs = tokens.astype(jnp.float32)
    normed = rms_scale(inputs, gain_in).astype(jnp.bfloat16)
    unit_rows = jnp.dot(normed, proj_in, preferred_element_type=jnp.float32).astype(jnp.bfloat16)
    branch, new_real, new_imag = state_step(unit_rows, state_real, state_imag, decay_rate, frequency, log_step, input_real, input_imag, output_real, output_imag, skip_gain)
    residual = inputs + jnp.dot(branch, proj_out, preferred_element_type=jnp.float32)
    mixed = rms_scale(residual, gain_mid).astype(jnp.bfloat16)
    weights = jnp.exp(route_logits)
    weights = weights / lax.optimization_barrier(jnp.sum(weights, axis=1, keepdims=True))
    limit_rows = N_EP * CAP
    expert_count = expert_gate.shape[0]

    def one_expert(running, expert_index):
        shares = lax.optimization_barrier(jnp.sum(jnp.where(routes == expert_index, weights, 0.0), axis=1))
        marked = jnp.any(routes == expert_index, axis=1).astype(jnp.int32)
        order_rows = jnp.argsort(1 - marked, stable=True)[:limit_rows].astype(jnp.int32)
        picked = jnp.take(mixed, order_rows, axis=0)
        result = expert_apply(picked, expert_gate[expert_index], expert_up[expert_index], expert_down[expert_index])
        running = running.at[order_rows].add(shares[order_rows][:, None] * result.astype(jnp.float32))
        return (running, None)
    routed, _ = lax.scan(one_expert, jnp.zeros(residual.shape, jnp.float32), jnp.arange(expert_count, dtype=jnp.int32))
    hidden = (jax.nn.silu(jnp.dot(mixed, dense_gate, preferred_element_type=jnp.float32)) * jnp.dot(mixed, dense_up, preferred_element_type=jnp.float32)).astype(jnp.bfloat16)
    dense_out = jnp.dot(hidden, dense_down, preferred_element_type=jnp.float32)
    gate_logit = jnp.dot(hidden.astype(jnp.float32), dense_mix, precision=HIGH)
    layer_out = (residual + routed + jax.nn.sigmoid(gate_logit)[:, None] * dense_out).astype(jnp.bfloat16)
    return (layer_out, new_real, new_imag)
```

```python
import functools

import jax
import jax.numpy as jnp
from jax import lax
from jax.experimental import pallas as pl
from jax.experimental.pallas import tpu as pltpu
from jax.sharding import PartitionSpec as P

EPS = 1e-06
LIMIT = 7.0
ALPHA = 1.702
HIGH = lax.Precision.HIGHEST


def rms_scale(values, gain_vec):
    return values * lax.rsqrt(jnp.mean(values * values, axis=-1, keepdims=True) + EPS) * gain_vec


def state_step(
    unit_rows,
    state_real,
    state_imag,
    decay_rate,
    frequency,
    log_step,
    input_real,
    input_imag,
    output_real,
    output_imag,
    skip_gain,
):
    seq_count = unit_rows.shape[0]
    groups, group_size = skip_gain.shape
    inputs = unit_rows.astype(jnp.float32).reshape(seq_count, groups, group_size)
    step_size = jnp.exp(log_step)[:, None]
    decay_part = -decay_rate
    magnitude = jnp.exp(decay_part * step_size)
    carry_real = magnitude * jnp.cos(frequency * step_size)
    carry_imag = magnitude * jnp.sin(frequency * step_size)
    denom = decay_part * decay_part + frequency * frequency
    feed_real = ((carry_real - 1.0) * decay_part + carry_imag * frequency) / denom
    feed_imag = (carry_imag * decay_part - (carry_real - 1.0) * frequency) / denom
    drive_real = jnp.einsum("sgp,gnp->sgn", inputs, input_real, precision=HIGH)
    drive_imag = jnp.einsum("sgp,gnp->sgn", inputs, input_imag, precision=HIGH)
    new_real = (
        carry_real * state_real
        - carry_imag * state_imag
        + feed_real * drive_real
        - feed_imag * drive_imag
    )
    new_imag = (
        carry_real * state_imag
        + carry_imag * state_real
        + feed_real * drive_imag
        + feed_imag * drive_real
    )
    readout = (
        jnp.einsum("gpn,sgn->sgp", output_real, new_real, precision=HIGH)
        - jnp.einsum("gpn,sgn->sgp", output_imag, new_imag, precision=HIGH)
        + skip_gain * inputs
    )
    branch = jax.nn.gelu(readout).reshape(seq_count, groups * group_size).astype(jnp.bfloat16)
    return (branch, new_real, new_imag)


def expert_apply(row_block, gate_weight, up_weight, down_weight):
    gated = jnp.minimum(jnp.dot(row_block, gate_weight, preferred_element_type=jnp.float32), LIMIT)
    upper = jnp.clip(
        jnp.dot(row_block, up_weight, preferred_element_type=jnp.float32), -LIMIT, LIMIT
    )
    activated = ((upper + 1.0) * gated * jax.nn.sigmoid(ALPHA * gated)).astype(jnp.bfloat16)
    return jnp.dot(activated, down_weight, preferred_element_type=jnp.float32).astype(jnp.bfloat16)


def spot(n):
    me = lax.axis_index("ep")
    return me, me // 4, (me // 2) % 2, me % 2, n // 4


def index_of(hi, mid, lo):
    return hi * 4 + mid * 2 + lo


def greet(peers):
    barrier = pltpu.get_barrier_semaphore()
    for peer in peers:
        pl.semaphore_signal(
            barrier, inc=1, device_id={"ep": peer}, device_id_type=pl.DeviceIdType.MESH
        )
    pl.semaphore_wait(barrier, len(peers))


def remote(src, dst, send_sem, recv_sem, peer):
    return pltpu.make_async_remote_copy(
        src_ref=src,
        dst_ref=dst,
        send_sem=send_sem,
        recv_sem=recv_sem,
        device_id={"ep": peer},
        device_id_type=pl.DeviceIdType.MESH,
    )


def gather_kernel(n, x_ref, o_ref, send_sem, z_sem, y_sem, c_sem):
    me, hi, mid, lo, span = spot(n)
    core = index_of(hi, mid, 1 - lo)
    across = index_of(hi, 1 - mid, lo)
    ahead = [(hi + 1 + j) % span for j in range(span - 1)]
    behind = [(hi + span - 1 - j) % span for j in range(span - 1)]
    greet([core, across] + [index_of(h, mid, lo) for h in ahead])
    sent = []

    def push(src, slot, sem, peer):
        copy = remote(src, o_ref.at[slot], send_sem.at[len(sent)], sem, peer)
        copy.start()
        sent.append(copy)
        return copy

    z_copies = [
        push(x_ref, me, z_sem.at[j], index_of(ahead[j], mid, lo)) for j in range(span - 1)
    ]
    y_copies = [push(x_ref, me, y_sem.at[0], across)]
    c_copies = [push(x_ref, me, c_sem.at[0], core)]
    o_ref[me] = x_ref[...]
    for j in range(span):
        if j < span - 1:
            z_copies[j].wait_recv()
            slot = index_of(behind[j], mid, lo)
            y_copies.append(push(o_ref.at[slot], slot, y_sem.at[j + 1], across))
            c_copies.append(push(o_ref.at[slot], slot, c_sem.at[j + 1], core))
        y_copies[j].wait_recv()
        slot = index_of(hi if j == 0 else behind[j - 1], 1 - mid, lo)
        c_copies.append(push(o_ref.at[slot], slot, c_sem.at[span + j], core))
    for copy in c_copies:
        copy.wait_recv()
    for copy in sent:
        copy.wait_send()


def gather_rows(x, n, collective_id):
    rows, width = x.shape
    span = n // 4
    out = pl.pallas_call(
        functools.partial(gather_kernel, n),
        out_shape=jax.ShapeDtypeStruct((n, rows, width), x.dtype),
        in_specs=[pl.BlockSpec(memory_space=pltpu.VMEM)],
        out_specs=pl.BlockSpec(memory_space=pltpu.VMEM),
        scratch_shapes=[
            pltpu.SemaphoreType.DMA((4 * span,)),
            pltpu.SemaphoreType.DMA((span,)),
            pltpu.SemaphoreType.DMA((span,)),
            pltpu.SemaphoreType.DMA((2 * span,)),
        ],
        compiler_params=pltpu.CompilerParams(
            collective_id=collective_id, has_side_effects=True
        ),
        name=f"gather_{collective_id}",
    )(x)
    return out.reshape(n * rows, width)


def scatter_kernel(
    n, x_ref, o_ref, c_buf, y_out, y_buf, z_out, z_buf, send_sem, c_sem, y_sem, z_sem
):
    me, hi, mid, lo, span = spot(n)
    core = index_of(hi, mid, 1 - lo)
    across = index_of(hi, 1 - mid, lo)
    order = [(hi + 1 + j) % span for j in range(span)]
    greet([core, across] + [index_of(h, mid, lo) for h in order[:-1]])
    sent = []

    def push(src, dst, sem, peer):
        copy = remote(src, dst, send_sem.at[len(sent)], sem, peer)
        copy.start()
        sent.append(copy)
        return copy

    c_copies = []
    for turn, side in enumerate((1 - mid, mid)):
        for j in range(span):
            at = turn * span + j
            c_copies.append(
                push(
                    x_ref.at[index_of(order[j], side, 1 - lo)], c_buf.at[at], c_sem.at[at], core
                )
            )
    y_copies = []
    for j in range(span):
        c_copies[j].wait_recv()
        own = x_ref[index_of(order[j], 1 - mid, lo)].astype(jnp.float32)
        y_out[j] = (own + c_buf[j].astype(jnp.float32)).astype(y_out.dtype)
        y_copies.append(push(y_out.at[j], y_buf.at[j], y_sem.at[j], across))
    z_copies = []
    total = None
    for j in range(span):
        c_copies[span + j].wait_recv()
        y_copies[j].wait_recv()
        value = (
            x_ref[index_of(order[j], mid, lo)].astype(jnp.float32)
            + c_buf[span + j].astype(jnp.float32)
            + y_buf[j].astype(jnp.float32)
        )
        if j < span - 1:
            z_out[j] = value.astype(z_out.dtype)
            z_copies.append(
                push(z_out.at[j], z_buf.at[j], z_sem.at[j], index_of(order[j], mid, lo))
            )
        else:
            o_ref[...] = value
    for j in range(span - 1):
        z_copies[j].wait_recv()
        o_ref[...] += z_buf[j].astype(jnp.float32)
    for copy in sent:
        copy.wait_send()


def scatter_rows(x, n, collective_id):
    rows, width = x.shape[0] // n, x.shape[1]
    span = n // 4
    block = (rows, width)
    return pl.pallas_call(
        functools.partial(scatter_kernel, n),
        out_shape=jax.ShapeDtypeStruct(block, jnp.float32),
        in_specs=[pl.BlockSpec(memory_space=pltpu.VMEM)],
        out_specs=pl.BlockSpec(memory_space=pltpu.VMEM),
        scratch_shapes=[
            pltpu.VMEM((2 * span,) + block, x.dtype),
            pltpu.VMEM((span,) + block, x.dtype),
            pltpu.VMEM((span,) + block, x.dtype),
            pltpu.VMEM((span,) + block, x.dtype),
            pltpu.VMEM((span,) + block, x.dtype),
            pltpu.SemaphoreType.DMA((4 * span,)),
            pltpu.SemaphoreType.DMA((2 * span,)),
            pltpu.SemaphoreType.DMA((span,)),
            pltpu.SemaphoreType.DMA((span,)),
        ],
        compiler_params=pltpu.CompilerParams(
            collective_id=collective_id, has_side_effects=True
        ),
        name=f"scatter_{collective_id}",
    )(x.reshape((n,) + block))


def total_kernel(n, x_ref, o_ref, buf, send_sem, recv_sem):
    me = lax.axis_index("ep")
    peers = [(me + 1 + j) % n for j in range(n - 1)]
    greet(peers)
    copies = [
        remote(x_ref, buf.at[j], send_sem.at[j], recv_sem.at[j], peers[j]) for j in range(n - 1)
    ]
    for copy in copies:
        copy.start()
    value = x_ref[...]
    for j in range(n - 1):
        copies[j].wait_recv()
        value = value + buf[j]
    o_ref[...] = value
    for copy in copies:
        copy.wait_send()


def total_over(x, n, collective_id):
    lanes = x.reshape(-1, 128)
    out = pl.pallas_call(
        functools.partial(total_kernel, n),
        out_shape=jax.ShapeDtypeStruct(lanes.shape, lanes.dtype),
        in_specs=[pl.BlockSpec(memory_space=pltpu.VMEM)],
        out_specs=pl.BlockSpec(memory_space=pltpu.VMEM),
        scratch_shapes=[
            pltpu.VMEM((n - 1,) + lanes.shape, lanes.dtype),
            pltpu.SemaphoreType.DMA((n - 1,)),
            pltpu.SemaphoreType.DMA((n - 1,)),
        ],
        compiler_params=pltpu.CompilerParams(
            collective_id=collective_id, has_side_effects=True
        ),
        name=f"total_{collective_id}",
    )(lanes)
    return out.reshape(x.shape)


def dense_hidden(row_block, dense_gate, dense_up):
    return (
        jax.nn.silu(jnp.dot(row_block, dense_gate, preferred_element_type=jnp.float32))
        * jnp.dot(row_block, dense_up, preferred_element_type=jnp.float32)
    ).astype(jnp.bfloat16)


def on_device(
    tokens,
    routes,
    route_logits,
    state_real,
    state_imag,
    gain_in,
    proj_in,
    decay_rate,
    frequency,
    log_step,
    input_real,
    input_imag,
    output_real,
    output_imag,
    skip_gain,
    proj_out,
    gain_mid,
    expert_gate,
    expert_up,
    expert_down,
    dense_gate,
    dense_up,
    dense_down,
    dense_mix,
):
    devices = lax.axis_size("ep")
    me = lax.axis_index("ep")
    own_rows, width = tokens.shape
    top_count = routes.shape[1]
    capacity = max(2, 2 * own_rows * top_count // devices)
    inputs = tokens.astype(jnp.float32)
    normed = rms_scale(inputs, gain_in).astype(jnp.bfloat16)
    unit_rows = jnp.dot(
        gather_rows(normed, devices, 0), proj_in, preferred_element_type=jnp.float32
    ).astype(jnp.bfloat16)
    branch, new_real, new_imag = state_step(
        unit_rows,
        state_real,
        state_imag,
        decay_rate,
        frequency,
        log_step,
        input_real,
        input_imag,
        output_real,
        output_imag,
        skip_gain,
    )
    mixer_part = jnp.dot(branch, proj_out, preferred_element_type=jnp.float32)
    residual = inputs + scatter_rows(mixer_part.astype(jnp.bfloat16), devices, 1)
    mixed = rms_scale(residual, gain_mid).astype(jnp.bfloat16)
    weights = jnp.exp(route_logits)
    weights = weights / jnp.sum(weights, axis=1, keepdims=True)
    expert_ids = jnp.arange(devices, dtype=jnp.int32)
    named = routes[:, :, None] == expert_ids[None, None, :]
    table = jnp.sum(jnp.where(named, weights[:, :, None], 0.0), axis=1)
    coarse = table.astype(jnp.bfloat16)
    fine = (table - coarse.astype(jnp.float32)).astype(jnp.bfloat16)
    spare = jnp.zeros((own_rows, -(2 * devices) % 128), jnp.bfloat16)
    gathered = gather_rows(jnp.concatenate([mixed, coarse, fine, spare], axis=1), devices, 2)
    all_mixed = gathered[:, :width]
    hidden = dense_hidden(all_mixed, dense_gate, dense_up)
    logit_term = jnp.dot(hidden.astype(jnp.float32), dense_mix, precision=HIGH)
    gate_logit = total_over(logit_term, devices, 3)
    dense_term = jnp.dot(hidden, dense_down, preferred_element_type=jnp.float32)
    mine = (expert_ids == me)[None, :]
    extra = gathered[:, width:].astype(jnp.float32)
    share = jnp.sum(
        jnp.where(mine, extra[:, :devices] + extra[:, devices : 2 * devices], 0.0), axis=1
    ).reshape(devices, own_rows)
    taken = share > 0.0
    slot = jnp.cumsum(taken.astype(jnp.int32), axis=1) - 1
    slot = jnp.where(taken, slot + expert_ids[:, None] * capacity, -1).reshape(-1)
    slot_ids = jnp.arange(devices * capacity, dtype=jnp.int32)
    picks = slot[None, :] == slot_ids[:, None]
    places = slot[:, None] == slot_ids[None, :]
    flat_rows = jnp.dot(
        picks.astype(jnp.bfloat16), all_mixed, preferred_element_type=jnp.float32
    ).astype(jnp.bfloat16)
    result = expert_apply(flat_rows, expert_gate[0], expert_up[0], expert_down[0])
    slot_share = jnp.sum(jnp.where(picks, share.reshape(1, -1), 0.0), axis=1, keepdims=True)
    scaled = (result.astype(jnp.float32) * slot_share).astype(jnp.bfloat16)
    routed = jnp.dot(places.astype(jnp.bfloat16), scaled, preferred_element_type=jnp.float32)
    part = (routed + jax.nn.sigmoid(gate_logit)[:, None] * dense_term).astype(jnp.bfloat16)
    layer_out = (residual + scatter_rows(part, devices, 4)).astype(jnp.bfloat16)
    return (layer_out, new_real, new_imag)


def solution(mesh):
    in_specs = (
        P(("grp", "ep"), None),
        P(("grp", "ep"), None),
        P(("grp", "ep"), None),
        P("grp", "ep", None),
        P("grp", "ep", None),
        P(),
        P(None, "ep"),
        P("ep", None),
        P("ep", None),
        P("ep"),
        P("ep", None, None),
        P("ep", None, None),
        P("ep", None, None),
        P("ep", None, None),
        P("ep", None),
        P("ep", None),
        P(),
        P("ep", None, None),
        P("ep", None, None),
        P("ep", None, None),
        P(None, "ep"),
        P(None, "ep"),
        P("ep", None),
        P("ep"),
    )
    out_specs = (P(("grp", "ep"), None), P("grp", "ep", None), P("grp", "ep", None))
    return jax.shard_map(
        on_device, mesh=mesh, in_specs=in_specs, out_specs=out_specs, check_vma=False
    )
```

```python
import functools

import jax
import jax.numpy as jnp
from jax import lax
from jax.experimental import pallas as pl
from jax.experimental.pallas import tpu as pltpu
from jax.sharding import PartitionSpec as P

EPS = 1e-06
LIMIT = 7.0
ALPHA = 1.702
HIGH = lax.Precision.HIGHEST


def rms_scale(values, gain_vec):
    return values * lax.rsqrt(jnp.mean(values * values, axis=-1, keepdims=True) + EPS) * gain_vec


def state_step(
    unit_rows,
    state_real,
    state_imag,
    decay_rate,
    frequency,
    log_step,
    input_real,
    input_imag,
    output_real,
    output_imag,
    skip_gain,
):
    seq_count = unit_rows.shape[0]
    groups, group_size = skip_gain.shape
    inputs = unit_rows.astype(jnp.float32).reshape(seq_count, groups, group_size)
    step_size = jnp.exp(log_step)[:, None]
    decay_part = -decay_rate
    magnitude = jnp.exp(decay_part * step_size)
    carry_real = magnitude * jnp.cos(frequency * step_size)
    carry_imag = magnitude * jnp.sin(frequency * step_size)
    denom = decay_part * decay_part + frequency * frequency
    feed_real = ((carry_real - 1.0) * decay_part + carry_imag * frequency) / denom
    feed_imag = (carry_imag * decay_part - (carry_real - 1.0) * frequency) / denom
    drive_real = jnp.einsum("sgp,gnp->sgn", inputs, input_real, precision=HIGH)
    drive_imag = jnp.einsum("sgp,gnp->sgn", inputs, input_imag, precision=HIGH)
    new_real = (
        carry_real * state_real
        - carry_imag * state_imag
        + feed_real * drive_real
        - feed_imag * drive_imag
    )
    new_imag = (
        carry_real * state_imag
        + carry_imag * state_real
        + feed_real * drive_imag
        + feed_imag * drive_real
    )
    readout = (
        jnp.einsum("gpn,sgn->sgp", output_real, new_real, precision=HIGH)
        - jnp.einsum("gpn,sgn->sgp", output_imag, new_imag, precision=HIGH)
        + skip_gain * inputs
    )
    branch = jax.nn.gelu(readout).reshape(seq_count, groups * group_size).astype(jnp.bfloat16)
    return (branch, new_real, new_imag)


def expert_apply(row_block, gate_weight, up_weight, down_weight):
    gated = jnp.minimum(jnp.dot(row_block, gate_weight, preferred_element_type=jnp.float32), LIMIT)
    upper = jnp.clip(
        jnp.dot(row_block, up_weight, preferred_element_type=jnp.float32), -LIMIT, LIMIT
    )
    activated = ((upper + 1.0) * gated * jax.nn.sigmoid(ALPHA * gated)).astype(jnp.bfloat16)
    return jnp.dot(activated, down_weight, preferred_element_type=jnp.float32).astype(jnp.bfloat16)


def spot(n):
    me = lax.axis_index("ep")
    return me, me // 4, (me // 2) % 2, me % 2, n // 4


def index_of(hi, mid, lo):
    return hi * 4 + mid * 2 + lo


def greet(peers, work=lambda: None):
    barrier = pltpu.get_barrier_semaphore()
    for peer in peers:
        pl.semaphore_signal(
            barrier, inc=1, device_id={"ep": peer}, device_id_type=pl.DeviceIdType.MESH
        )
    result = work()
    pl.semaphore_wait(barrier, len(peers))
    return result


def remote(src, dst, send_sem, recv_sem, peer):
    return pltpu.make_async_remote_copy(
        src_ref=src,
        dst_ref=dst,
        send_sem=send_sem,
        recv_sem=recv_sem,
        device_id={"ep": peer},
        device_id_type=pl.DeviceIdType.MESH,
    )


class Lane:
    def __init__(self, send_sem, recv_sem):
        self.send_sem, self.recv_sem, self.copies = send_sem, recv_sem, []

    def push(self, src, dst, peer):
        at = len(self.copies)
        copy = remote(src, dst, self.send_sem.at[at], self.recv_sem.at[at], peer)
        copy.start()
        self.copies.append(copy)
        return copy

    def finish(self):
        for copy in self.copies:
            copy.wait_send()


def ring_rows(step, limit, way, rows):
    if step < limit:
        return pl.ds(0, rows)
    return pl.ds(0, rows // 2) if way == 1 else pl.ds(rows // 2, rows - rows // 2)


def neighbours(n):
    me, hi, mid, lo, span = spot(n)
    return [
        index_of(hi, mid, 1 - lo),
        index_of(hi, 1 - mid, lo),
        index_of((hi + 1) % span, mid, lo),
        index_of((hi + span - 1) % span, mid, lo),
    ]


def spread(n, lane, x, o):
    me, hi, mid, lo, span = spot(n)
    core, across, right, left = neighbours(n)
    ways = {1: right, -1: left}
    rows, width = x.shape
    limit = span // 2
    cut = width // 256 * 128
    first, second = pl.ds(0, cut), pl.ds(cut, width - cut)
    whole, full = pl.ds(0, width), pl.ds(0, rows)
    ends = []

    def relay(slot, at_rows, at_columns, peer):
        part = o.at[slot, at_rows, at_columns]
        return lane.push(part, part, peer)

    partner = lane.push(x.at[:, second], o.at[me, :, second], across)
    own = {way: lane.push(x, o.at[me], peer) for way, peer in ways.items()}
    crossed = [
        (
            lane.push(x.at[:, first], o.at[me, :, first], across),
            index_of(hi, 1 - mid, lo),
            full,
        )
    ]
    ends.append(lane.push(x, o.at[me], core))
    o[me] = x[...]
    partner.wait_recv()
    other = {way: relay(across, full, second, peer) for way, peer in ways.items()}
    ends.append(relay(across, full, second, core))
    for step in range(1, limit + 1):
        for way, peer in ways.items():
            own[way].wait_recv()
            h = (hi + span - way * step) % span
            slot = index_of(h, mid, lo)
            at_rows = ring_rows(step, limit, way, rows)
            if step < limit:
                own[way] = relay(slot, ring_rows(step + 1, limit, way, rows), whole, peer)
            crossed.append(
                (relay(slot, at_rows, first, across), index_of(h, 1 - mid, lo), at_rows)
            )
            ends.append(relay(slot, at_rows, whole, core))
        for way, peer in ways.items():
            other[way].wait_recv()
            slot = index_of((hi + span - way * step) % span, 1 - mid, lo)
            at_rows = ring_rows(step, limit, way, rows)
            if step < limit:
                other[way] = relay(slot, ring_rows(step + 1, limit, way, rows), second, peer)
            ends.append(relay(slot, at_rows, second, core))
    for copy, slot, at_rows in crossed:
        copy.wait_recv()
        ends.append(relay(slot, at_rows, first, core))
    for copy in ends:
        copy.wait_recv()


def reduce_to_own(n, lane, x, c_buf, part, y_buf, ring_buf, last_buf):
    me, hi, mid, lo, span = spot(n)
    core, across, right, left = neighbours(n)
    ways = {1: right, -1: left}
    rows, width = x.shape[1:]
    limit = span // 2
    cut = width // 256 * 128
    first, second = pl.ds(0, cut), pl.ds(cut, width - cut)
    order = [limit] + [j for j in range(span) if j not in (0, limit)] + [0]

    def add(slot, at_rows, at_columns, value):
        here = part[slot, at_rows, at_columns].astype(jnp.float32)
        part[slot, at_rows, at_columns] = (here + value.astype(jnp.float32)).astype(part.dtype)

    def send_on(base, target, way, at_columns, stream):
        at_rows = ring_rows(target, limit, way, rows)
        slot = base + (target if way == 1 else (span - target) % span)
        at = (0 if way == 1 else limit) + limit - target
        return lane.push(
            part.at[slot, at_rows, at_columns],
            ring_buf.at[stream, at, at_rows, at_columns],
            ways[way],
        )

    def take(base, target, way, at_columns, stream):
        at_rows = ring_rows(target + 1, limit, way, rows)
        slot = base + (target if way == 1 else (span - target) % span)
        at = (0 if way == 1 else limit) + limit - target - 1
        add(slot, at_rows, at_columns, ring_buf[stream, at, at_rows, at_columns])

    arrivals = {}
    for base, side in ((span, 1 - mid), (0, mid)):
        for j in order:
            block = x.at[index_of((hi + j) % span, side, 1 - lo)]
            arrivals[base + j] = lane.push(block, c_buf.at[base + j], core)

    def settle(base, side, j):
        arrivals[base + j].wait_recv()
        own = x[index_of((hi + j) % span, side, lo)].astype(jnp.float32)
        part[base + j] = (own + c_buf[base + j].astype(jnp.float32)).astype(part.dtype)

    chains, crossed = {}, {}
    for j in order:
        settle(span, 1 - mid, j)
        if j == limit:
            for way in ways:
                chains[0, way] = send_on(span, limit, way, second, 0)
        crossed[j] = lane.push(part.at[span + j, :, first], y_buf.at[j, :, first], across)
    for j in order:
        settle(0, mid, j)
        if j == limit:
            for way in ways:
                chains[1, way] = send_on(0, limit, way, second, 1)

    def advance(stream, base, at_columns, target):
        for way in ways:
            chains[stream, way].wait_recv()
            take(base, target, way, at_columns, stream)
            if target > 0:
                chains[stream, way] = send_on(base, target, way, at_columns, stream)

    def join(j):
        crossed[j].wait_recv()
        add(j, pl.ds(0, rows), first, y_buf[j, :, first])

    join(limit)
    for way in ways:
        chains[2, way] = send_on(0, limit, way, first, 2)
    for target in range(limit - 1, -1, -1):
        advance(0, span, second, target)
        if target == 0:
            last = lane.push(part.at[span, :, second], last_buf.at[:, second], across)
        advance(1, 0, second, target)
        for j in sorted({target, (span - target) % span}):
            join(j)
        advance(2, 0, first, target)
    last.wait_recv()
    add(0, pl.ds(0, rows), second, last_buf[:, second])


def lane_sems(n):
    return [pltpu.SemaphoreType.DMA((16 * n,)), pltpu.SemaphoreType.DMA((16 * n,))]


def reduce_scratch(n, block, dtype):
    span = n // 4
    return [
        pltpu.VMEM((2 * span,) + block, dtype),
        pltpu.VMEM((2 * span,) + block, dtype),
        pltpu.VMEM((span,) + block, dtype),
        pltpu.VMEM((3, span) + block, dtype),
        pltpu.VMEM(block, dtype),
    ]


def vmem_specs(count):
    return [pl.BlockSpec(memory_space=pltpu.VMEM)] * count


def arrival_order(span):
    return sorted(range(span - 1), key=lambda j: min(j + 1, span - 1 - j))


def spread_simple(n, lane, x, o):
    me, hi, mid, lo, span = spot(n)
    core, across, right, left = neighbours(n)
    ahead = [(hi + 1 + j) % span for j in range(span - 1)]
    behind = [(hi + span - 1 - j) % span for j in range(span - 1)]

    def relay(slot, peer):
        return lane.push(o.at[slot], o.at[slot], peer)

    z_copies = [lane.push(x, o.at[me], index_of(h, mid, lo)) for h in ahead]
    y_copies = [lane.push(x, o.at[me], across)]
    ends = [lane.push(x, o.at[me], core)]
    o[me] = x[...]
    for j in arrival_order(span):
        z_copies[j].wait_recv()
        slot = index_of(behind[j], mid, lo)
        y_copies.append(relay(slot, across))
        ends.append(relay(slot, core))
    slots = [hi] + [behind[j] for j in arrival_order(span)]
    for j in range(span):
        y_copies[j].wait_recv()
        ends.append(relay(index_of(slots[j], 1 - mid, lo), core))
    for copy in ends:
        copy.wait_recv()


def units_kernel(n, tokens_ref, gain_ref, weight_ref, o_ref, row_buf, all_buf, *sems):
    def norm():
        row_buf[...] = rms_scale(tokens_ref[...].astype(jnp.float32), gain_ref[...]).astype(
            row_buf.dtype
        )

    rows, width = tokens_ref.shape
    me, hi, mid, lo, span = spot(n)
    columns = [index_of((hi + 1 + j) % span, mid, lo) for j in range(span - 1)]
    core, across, right, left = neighbours(n)
    greet([core, across] + columns, norm)
    lane = Lane(*sems)
    spread_simple(n, lane, row_buf, all_buf)
    for i in range(4):
        part = n // 4
        here = all_buf[i * part : (i + 1) * part].reshape(part * rows, width)
        o_ref[:, i * part * rows : (i + 1) * part * rows] = lax.dot_general(
            weight_ref[...],
            here,
            (((1,), (1,)), ((), ())),
            preferred_element_type=jnp.float32,
        ).astype(o_ref.dtype)
    lane.finish()


def gather_units(tokens, gain, weight, n, collective_id):
    rows, width = tokens.shape
    return pl.pallas_call(
        functools.partial(units_kernel, n),
        out_shape=jax.ShapeDtypeStruct((weight.shape[1], n * rows), jnp.bfloat16),
        in_specs=vmem_specs(3),
        out_specs=vmem_specs(1)[0],
        scratch_shapes=[
            pltpu.VMEM((rows, width), jnp.bfloat16),
            pltpu.VMEM((n, rows, width), jnp.bfloat16),
        ]
        + lane_sems(n),
        compiler_params=pltpu.CompilerParams(
            collective_id=collective_id, has_side_effects=True
        ),
        name=f"units_{collective_id}",
    )(tokens, gain.reshape(1, -1), weight.T).T


def scatter_kernel(n, x_ref, own_ref, o_ref, c_buf, part, y_buf, ring_buf, last_buf, *sems):
    greet(neighbours(n))
    lane = Lane(*sems)
    reduce_to_own(n, lane, x_ref, c_buf, part, y_buf, ring_buf, last_buf)
    o_ref[...] = (own_ref[...] + part[0].astype(jnp.float32)).astype(o_ref.dtype)
    lane.finish()


def scatter_rows(x, own, n, collective_id):
    rows, width = own.shape
    block = (rows, width)
    return pl.pallas_call(
        functools.partial(scatter_kernel, n),
        out_shape=jax.ShapeDtypeStruct(block, jnp.bfloat16),
        in_specs=vmem_specs(2),
        out_specs=vmem_specs(1)[0],
        scratch_shapes=reduce_scratch(n, block, x.dtype) + lane_sems(n),
        compiler_params=pltpu.CompilerParams(
            collective_id=collective_id, has_side_effects=True
        ),
        name=f"scatter_{collective_id}",
    )(x.reshape((n,) + block), own)


def middle_kernel(
    n,
    x_ref,
    tokens_ref,
    gain_ref,
    routes_ref,
    scores_ref,
    gate_ref,
    up_ref,
    mix_ref,
    all_ref,
    residual_ref,
    hidden_ref,
    logit_ref,
    c_buf,
    part,
    y_buf,
    ring_buf,
    last_buf,
    row_buf,
    logit_own,
    logit_buf,
    *sems,
):
    me = lax.axis_index("ep")
    peers = [(me + 1 + j) % n for j in range(n - 1)]
    rows, width = tokens_ref.shape

    def share_table():
        weights = jnp.exp(scores_ref[...])
        weights = weights / jnp.sum(weights, axis=1, keepdims=True)
        spare = row_buf.shape[1] - width
        ids = lax.broadcasted_iota(jnp.int32, (rows, spare), 1)
        expert = ids % n
        table = jnp.zeros((rows, spare), jnp.float32)
        for k in range(weights.shape[1]):
            hit = routes_ref[:, k : k + 1] == expert
            table = table + jnp.where(hit, weights[:, k : k + 1], 0.0)
        coarse = table.astype(row_buf.dtype).astype(jnp.float32)
        value = jnp.where(ids < n, coarse, jnp.where(ids < 2 * n, table - coarse, 0.0))
        row_buf[:, width:] = value.astype(row_buf.dtype)

    greet(peers, share_table)
    lane = Lane(*sems)
    reduce_to_own(n, lane, x_ref, c_buf, part, y_buf, ring_buf, last_buf)
    residual = tokens_ref[...].astype(jnp.float32) + part[0].astype(jnp.float32)
    residual_ref[...] = residual
    row_buf[:, :width] = rms_scale(residual, gain_ref[...]).astype(row_buf.dtype)
    spread(n, lane, row_buf, all_ref)
    chunk = 128 // rows
    total = jnp.zeros(logit_own.shape, jnp.float32)
    mix_shape = (logit_own.shape[0], mix_ref.shape[1])
    row_ids = lax.broadcasted_iota(jnp.int32, mix_shape, 0)
    for i in range(n // chunk):
        here = all_ref[i * chunk : (i + 1) * chunk, :, :width].reshape(128, width)
        hidden = dense_hidden(here, gate_ref[...], up_ref[...])
        hidden_ref[i * 128 : (i + 1) * 128] = hidden
        chosen = jnp.where(row_ids == i, mix_ref[...], 0.0)
        total = total + lax.dot_general(
            chosen,
            hidden.astype(jnp.float32),
            (((1,), (1,)), ((), ())),
            precision=HIGH,
            preferred_element_type=jnp.float32,
        )
    logit_own[...] = total
    copies = [lane.push(logit_own, logit_buf.at[j], peers[j]) for j in range(n - 1)]
    for j in range(n - 1):
        copies[j].wait_recv()
        total = total + logit_buf[j]
    logit_ref[...] = total
    lane.finish()


def middle(part, tokens, gain_mid, routes, scores, dense_gate, dense_up, dense_mix, n, collective_id):
    rows, width = tokens.shape
    block = (rows, width)
    wide = width + -(-(2 * n) // 128) * 128
    units = dense_gate.shape[1]
    logit_shape = (-(-(n * rows) // 1024) * 8, 128)
    gathered, residual, hidden, logits = pl.pallas_call(
        functools.partial(middle_kernel, n),
        out_shape=[
            jax.ShapeDtypeStruct((n, rows, wide), jnp.bfloat16),
            jax.ShapeDtypeStruct(block, jnp.float32),
            jax.ShapeDtypeStruct((n * rows, units), jnp.bfloat16),
            jax.ShapeDtypeStruct(logit_shape, jnp.float32),
        ],
        in_specs=vmem_specs(8),
        out_specs=vmem_specs(4),
        scratch_shapes=reduce_scratch(n, block, part.dtype)
        + [
            pltpu.VMEM((rows, wide), jnp.bfloat16),
            pltpu.VMEM(logit_shape, jnp.float32),
            pltpu.VMEM((n - 1,) + logit_shape, jnp.float32),
        ]
        + lane_sems(n),
        compiler_params=pltpu.CompilerParams(
            collective_id=collective_id, has_side_effects=True
        ),
        name=f"middle_{collective_id}",
    )(
        part.reshape((n,) + block),
        tokens,
        gain_mid.reshape(1, -1),
        routes,
        scores,
        dense_gate,
        dense_up,
        dense_mix.reshape(1, -1),
    )
    return (
        gathered.reshape(n * rows, wide),
        residual,
        hidden,
        logits.reshape(-1)[: n * rows],
    )


def dense_hidden(row_block, dense_gate, dense_up):
    return (
        jax.nn.silu(jnp.dot(row_block, dense_gate, preferred_element_type=jnp.float32))
        * jnp.dot(row_block, dense_up, preferred_element_type=jnp.float32)
    ).astype(jnp.bfloat16)


def on_device(
    tokens,
    routes,
    route_logits,
    state_real,
    state_imag,
    gain_in,
    proj_in,
    decay_rate,
    frequency,
    log_step,
    input_real,
    input_imag,
    output_real,
    output_imag,
    skip_gain,
    proj_out,
    gain_mid,
    expert_gate,
    expert_up,
    expert_down,
    dense_gate,
    dense_up,
    dense_down,
    dense_mix,
):
    devices = lax.axis_size("ep")
    me = lax.axis_index("ep")
    own_rows, width = tokens.shape
    top_count = routes.shape[1]
    capacity = max(2, 2 * own_rows * top_count // devices)
    unit_rows = gather_units(tokens, gain_in, proj_in, devices, 0)
    branch, new_real, new_imag = state_step(
        unit_rows,
        state_real,
        state_imag,
        decay_rate,
        frequency,
        log_step,
        input_real,
        input_imag,
        output_real,
        output_imag,
        skip_gain,
    )
    mixer_part = jnp.dot(branch, proj_out, preferred_element_type=jnp.float32)
    expert_ids = jnp.arange(devices, dtype=jnp.int32)
    gathered, residual, hidden, gate_logit = middle(
        mixer_part.astype(jnp.bfloat16),
        tokens,
        gain_mid,
        routes,
        route_logits,
        dense_gate,
        dense_up,
        dense_mix,
        devices,
        1,
    )
    all_mixed = gathered[:, :width]
    dense_term = jnp.dot(hidden, dense_down, preferred_element_type=jnp.float32)
    mine = (expert_ids == me)[None, :]
    extra = gathered[:, width:].astype(jnp.float32)
    share = jnp.sum(
        jnp.where(mine, extra[:, :devices] + extra[:, devices : 2 * devices], 0.0), axis=1
    ).reshape(devices, own_rows)
    taken = share > 0.0
    slot = jnp.cumsum(taken.astype(jnp.int32), axis=1) - 1
    slot = jnp.where(taken, slot + expert_ids[:, None] * capacity, -1).reshape(-1)
    slot_ids = jnp.arange(devices * capacity, dtype=jnp.int32)
    picks = slot[None, :] == slot_ids[:, None]
    places = slot[:, None] == slot_ids[None, :]
    flat_rows = jnp.dot(
        picks.astype(jnp.bfloat16), all_mixed, preferred_element_type=jnp.float32
    ).astype(jnp.bfloat16)
    result = expert_apply(flat_rows, expert_gate[0], expert_up[0], expert_down[0])
    slot_share = jnp.sum(jnp.where(picks, share.reshape(1, -1), 0.0), axis=1, keepdims=True)
    scaled = (result.astype(jnp.float32) * slot_share).astype(jnp.bfloat16)
    routed = jnp.dot(places.astype(jnp.bfloat16), scaled, preferred_element_type=jnp.float32)
    part = (routed + jax.nn.sigmoid(gate_logit)[:, None] * dense_term).astype(jnp.bfloat16)
    layer_out = scatter_rows(part, residual, devices, 2)
    return (layer_out, new_real, new_imag)


def solution(mesh):
    in_specs = (
        P(("grp", "ep"), None),
        P(("grp", "ep"), None),
        P(("grp", "ep"), None),
        P("grp", "ep", None),
        P("grp", "ep", None),
        P(),
        P(None, "ep"),
        P("ep", None),
        P("ep", None),
        P("ep"),
        P("ep", None, None),
        P("ep", None, None),
        P("ep", None, None),
        P("ep", None, None),
        P("ep", None),
        P("ep", None),
        P(),
        P("ep", None, None),
        P("ep", None, None),
        P("ep", None, None),
        P(None, "ep"),
        P(None, "ep"),
        P("ep", None),
        P("ep"),
    )
    out_specs = (P(("grp", "ep"), None), P("grp", "ep", None), P("grp", "ep", None))
    return jax.shard_map(
        on_device, mesh=mesh, in_specs=in_specs, out_specs=out_specs, check_vma=False
    )
```
